32 devices in a mesh: grp: 2 (over x), row: 4 (over z), col: 4 (over y, core).
Axes of the slice: x: 2, y: 2, z: 4, core: 2. Of those that a mesh axis runs over, the one named last changes fastest.
Arguments:
- gate_in: bfloat16 [8, 512, 1024], P(('grp', 'row'), 'col'), parts along dimension 0, may hold values from -6 to 6
- mult_in: bfloat16 [8, 512, 1024], P(('grp', 'row'), 'col'), parts along dimension 0, may hold values from -6 to 6
- value_in: bfloat16 [8, 512, 1024], P(('grp', 'row'), 'col'), parts along dimension 0, may hold values from -6 to 6
- taps_gate: float32 [3, 1024], replicated, may hold values from -3.5 to 3.5
- taps_mult: float32 [3, 1024], replicated, may hold values from -3.5 to 3.5
- taps_value: float32 [3, 1024], replicated, may hold values from -3.5 to 3.5
- filter_first: float32 [33, 128], replicated, may hold values from -3 to 3
- filter_second: float32 [128, 128], replicated, may hold values from -1 to 1
- filter_ahead: float32 [128, 1024], replicated, may hold values from -0.5 to 0.5
- filter_behind: float32 [128, 1024], replicated, may hold values from -0.5 to 0.5
- filter_decay: float32 [1024], replicated, may hold values from 0.05 to 17.033333
- skip_gain: float32 [1024], replicated, may hold values from -5 to 5
- out_weight: bfloat16 [1024, 2048], replicated, may hold values from -0.1875 to 0.1875
Outputs:
- mixed: bfloat16 [8, 512, 2048], P(('grp', 'row'), 'col'), parts along dimension 0
The draws below stay inside these ranges and needn't reach their ends.
There are 2 independent parts, one for each index of `grp`. The reference program is written for one: setup_inputs(seed, part) draws one part's arguments, and reference() takes and returns one part's arrays. A program takes and returns all parts, laid end to end along the dimension named above; an argument that names none is the same for every part. Nothing has to cross between parts.
All inputs are finite; a program needn't handle non-finite values.
Results may differ from the reference program's by a relative error of at most 0.0049.
Values may be sent and summed in bfloat16 or wider, within the bound.
A program may use at most 64 MiB of HBM per device.

```python
import math
import jax
import jax.numpy as jnp
from jax import lax

D = 2048
H = 1024
FH = 128
FEAT = 33
TAPS = 3
SEQ = 512
SEQS = 4


def draw_filter_decay(key, part):
    slow_key, fast_key, pick_key = jax.random.split(jax.random.fold_in(key, 7), 3)
    slow_rates = jnp.exp(jax.random.uniform(slow_key, (H,), jnp.float32, math.log(0.05), math.log(2.0)))
    fast_rates = (SEQ - 1) / jnp.exp(jax.random.uniform(fast_key, (H,), jnp.float32, math.log(30.0), math.log(100.0)))
    fast_share = 0.5
    chosen = jax.random.uniform(pick_key, (H,), jnp.float32) < fast_share
    return jnp.where(chosen, fast_rates, slow_rates)


def block_levels(key, shape, shards, low, high):
    level = 1.0
    for axis_at, parts in shards:
        heights = jax.random.uniform(jax.random.fold_in(jax.random.fold_in(key, 6), axis_at), (parts,), jnp.float32, low / len(shards), high / len(shards))
        level = level * jnp.repeat(jnp.exp(heights), shape[axis_at] // parts).reshape((-1,) + (1,) * (len(shape) - 1 - axis_at))
    return level


def gaussian(rng, extent, deviation, reach, cuts=(), kind=jnp.bfloat16):
    loudness = block_levels(rng, extent, cuts, -0.22, 0.18) if cuts else 1.0
    values = jax.random.normal(rng, extent, jnp.float32) * deviation * loudness
    return jnp.minimum(jnp.maximum(values, -reach), reach).astype(kind)


def setup_inputs(seed: int = 0, part: int = 0) -> dict:
    keys = jax.random.split(jax.random.key(seed), 14)
    own_keys = jax.random.split(jax.random.fold_in(keys[13], part), 14)
    return {
        "gate_in": gaussian(own_keys[0], (SEQS, SEQ, H), 1.0, 6.0, ((0, 4), (1, 4))),
        "mult_in": gaussian(own_keys[1], (SEQS, SEQ, H), 1.0, 6.0, ((0, 4), (1, 4))),
        "value_in": gaussian(own_keys[2], (SEQS, SEQ, H), 1.0, 6.0, ((0, 4), (1, 4))),
        "taps_gate": gaussian(keys[3], (TAPS, H), TAPS ** -0.5, 3.5, (), jnp.float32),
        "taps_mult": gaussian(keys[4], (TAPS, H), TAPS ** -0.5, 3.5, (), jnp.float32),
        "taps_value": gaussian(keys[5], (TAPS, H), TAPS ** -0.5, 3.5, (), jnp.float32),
        "filter_first": jnp.clip(jax.random.uniform(keys[6], (FEAT, FH), jnp.float32, -3.0, 3.0), -3.0, 3.0),
        "filter_second": jnp.clip(jax.random.uniform(keys[7], (FH, FH), jnp.float32, -1.0, 1.0), -1.0, 1.0),
        "filter_ahead": gaussian(keys[8], (FH, H), FH ** -0.5, 0.5, (), jnp.float32),
        "filter_behind": gaussian(keys[9], (FH, H), FH ** -0.5, 0.5, (), jnp.float32),
        "filter_decay": draw_filter_decay(jax.random.fold_in(keys[13], 71), part),
        "skip_gain": gaussian(keys[11], (H,), 1.0, 5.0, (), jnp.float32),
        "out_weight": gaussian(keys[12], (H, D), H ** -0.5, 0.1875),
    }


highest = lax.Precision.HIGHEST

def filter_hidden(mirror, seq_len, filter_first, filter_second):
    tau_values = mirror.astype(jnp.float32) / (seq_len - 1)
    omega_pos = 2.0 * math.pi / seq_len * mirror.astype(jnp.float32)
    band_count = (filter_first.shape[0] - 1) // 2
    band_values = jnp.linspace(0.0001, band_count - 1, band_count, dtype=jnp.float32)
    angles = omega_pos[:, None] * band_values[None, :]
    features = jnp.concatenate([tau_values[:, None], jnp.cos(angles), -jnp.sin(angles)], axis=1)
    hidden = jnp.sin(jnp.dot(features, filter_first, precision=highest))
    hidden = jnp.sin(jnp.dot(hidden, filter_second, precision=highest))
    return (hidden, tau_values)

def side_values(hidden, tau_values, side_weight, decay_rates):
    values = jnp.einsum('pf,fh->hp', hidden, side_weight, precision=highest)
    return values * jnp.exp(-decay_rates[:, None] * tau_values[None, :])

def short_conv(source, tap_weights):
    seq_len = source.shape[0]
    padded = jnp.pad(source.astype(jnp.float32), ((1, 1), (0, 0)))
    summed = jnp.zeros(source.shape, jnp.float32)
    for offset in range(tap_weights.shape[0]):
        summed = summed + tap_weights[offset] * padded[offset:offset + seq_len]
    return summed

def reference(gate_in, mult_in, value_in, taps_gate, taps_mult, taps_value, filter_first, filter_second, filter_ahead, filter_behind, filter_decay, skip_gain, out_weight):
    seq_len = gate_in.shape[1]
    span_len = 2 * seq_len
    mirror = jnp.arange(seq_len, dtype=jnp.int32)
    hidden, tau_values = filter_hidden(mirror, seq_len, filter_first, filter_second)
    ahead_vals = side_values(hidden, tau_values, filter_ahead, filter_decay)
    behind_vals = side_values(hidden, tau_values, filter_behind, filter_decay)
    kernel = jnp.concatenate([ahead_vals, jnp.zeros((ahead_vals.shape[0], 1), jnp.float32), jnp.flip(behind_vals[:, 1:], axis=1)], axis=1)
    kernel = kernel * lax.rsqrt(lax.optimization_barrier(jnp.sum(kernel * kernel, axis=1, keepdims=True)) + 1e-06)
    kernel_freq = jnp.fft.rfft(kernel, n=span_len, axis=1)

    def one_sequence(inputs):
        gate_rows, mult_rows, value_rows = inputs
        gate_part = short_conv(gate_rows, taps_gate)
        product = short_conv(value_rows, taps_value) * short_conv(mult_rows, taps_mult)
        spectrum = jnp.fft.rfft(product.T, n=span_len, axis=1)
        convolved = jnp.fft.irfft(spectrum * kernel_freq, n=span_len, axis=1)[:, :seq_len].T
        mixed_rows = ((convolved + skip_gain * product) * gate_part).astype(jnp.bfloat16)
        return jnp.dot(mixed_rows, out_weight, preferred_element_type=jnp.float32).astype(jnp.bfloat16)
    return lax.map(one_sequence, (gate_in, mult_in, value_in))
```

```python
import functools
import math

import jax
import jax.numpy as jnp
import numpy as np
from jax import lax
from jax.experimental import pallas as pl
from jax.experimental.pallas import tpu as pltpu
from jax.sharding import PartitionSpec as P

highest = lax.Precision.HIGHEST


def padded_2(shard, sides, width):
    for axis, dim in sides:
        size, length = (lax.axis_size(axis), shard.shape[dim])
        up = [(i, (i + 1) % size) for i in range(size - 1)]
        down = [(j, i) for i, j in up]
        last = lax.slice_in_dim(shard, length - width, length, axis=dim)
        leading = lax.slice_in_dim(shard, 0, width, axis=dim)
        before = lax.ppermute(last, axis, up)
        after = lax.ppermute(leading, axis, down)
        shard = jnp.concatenate([before, shard, after], axis=dim)
    return shard


def filter_hidden(mirror, seq_len, filter_first, filter_second):
    tau_values = mirror.astype(jnp.float32) / (seq_len - 1)
    omega_pos = 2.0 * math.pi / seq_len * mirror.astype(jnp.float32)
    band_count = (filter_first.shape[0] - 1) // 2
    band_values = jnp.linspace(0.0001, band_count - 1, band_count, dtype=jnp.float32)
    angles = omega_pos[:, None] * band_values[None, :]
    features = jnp.concatenate([tau_values[:, None], jnp.cos(angles), -jnp.sin(angles)], axis=1)
    hidden = jnp.sin(jnp.dot(features, filter_first, precision=highest))
    hidden = jnp.sin(jnp.dot(hidden, filter_second, precision=highest))
    return (hidden, tau_values)


def side_values(hidden, tau_values, side_weight, decay_rates):
    values = jnp.einsum("pf,fh->hp", hidden, side_weight, precision=highest)
    return values * jnp.exp(-decay_rates[:, None] * tau_values[None, :])


def angle_table(row_count, column_count, period):
    products = (
        lax.iota(jnp.int32, row_count)[:, None]
        * lax.iota(jnp.int32, column_count)[None, :]
        % period
    )
    angle = products.astype(jnp.float32) * (2.0 * math.pi / period)
    return (jnp.cos(angle), jnp.sin(angle))


def swap_halves(stacked, width):
    return jnp.concatenate([stacked[..., width:], stacked[..., :width]], axis=-1)


def forward(values, first_table, twist_even, twist_odd, second_block):
    channels, _, width = values.shape
    first = jnp.einsum("sfa,cab->cfsb", first_table, values, precision=highest)
    first = first.reshape(channels, first_table.shape[1], 2 * width)
    turned = first * twist_even + swap_halves(first, width) * twist_odd
    return jnp.einsum("cfk,kl->cfl", turned, second_block, precision=highest)


def inverse(spectrum, last_table, twist_even, twist_odd, second_block, span_len):
    channels, freq_rows, double_width = spectrum.shape
    width = double_width // 2
    back = jnp.einsum("cfk,kl->cfl", spectrum, second_block, precision=highest)
    turned = back * twist_even + swap_halves(back, width) * twist_odd
    turned = turned.reshape(channels, freq_rows, 2, width)
    result = jnp.einsum("asf,cfsb->cab", last_table, turned, precision=highest)
    return result / span_len


def spread_body(
    gate_in,
    mult_in,
    value_in,
    taps_gate,
    taps_mult,
    taps_value,
    filter_first,
    filter_second,
    filter_ahead,
    filter_behind,
    filter_decay,
    skip_gain,
    out_weight,
):
    col_count = lax.axis_size("col")
    col_index = lax.axis_index("col")
    tok_rows = gate_in.shape[1]
    seq_len = tok_rows * col_count
    span_len = 2 * seq_len
    group_size = filter_ahead.shape[1] // col_count
    stacked = jnp.stack([gate_in[0], mult_in[0], value_in[0]])
    padded = padded_2(stacked, (("col", 1),), 1).astype(jnp.float32)
    all_taps = jnp.stack([taps_gate, taps_mult, taps_value])
    shorted = jnp.zeros(stacked.shape, jnp.float32)
    for offset in range(all_taps.shape[1]):
        shorted = shorted + all_taps[:, offset][:, None, :] * padded[:, offset : offset + tok_rows]
    gate_part = shorted[0]
    product = shorted[2] * shorted[1]
    spread = lax.all_to_all(product.T, "col", split_axis=0, concat_axis=1, tiled=True)
    first_channel = col_index * group_size
    own_rates = lax.dynamic_slice_in_dim(filter_decay, first_channel, group_size)
    mirror = lax.iota(jnp.int32, seq_len)
    hidden, tau_values = filter_hidden(mirror, seq_len, filter_first, filter_second)
    ahead_vals = side_values(
        hidden,
        tau_values,
        lax.dynamic_slice_in_dim(filter_ahead, first_channel, group_size, 1),
        own_rates,
    )
    behind_vals = side_values(
        hidden,
        tau_values,
        lax.dynamic_slice_in_dim(filter_behind, first_channel, group_size, 1),
        own_rates,
    )
    kernel = jnp.concatenate(
        [ahead_vals, jnp.zeros((group_size, 1), jnp.float32), jnp.flip(behind_vals[:, 1:], axis=1)],
        axis=1,
    )
    kernel = kernel * lax.rsqrt(jnp.sum(kernel * kernel, axis=1, keepdims=True) + 1e-06)
    factor = 128
    half_rows = factor // 2
    width_second = span_len // factor
    first_cos, first_sin = angle_table(factor, factor, factor)
    twist_cos, twist_sin = angle_table(factor, width_second, span_len)
    second_cos, second_sin = angle_table(width_second, width_second, width_second)
    first_table = jnp.stack([first_cos, -first_sin])
    last_table = jnp.stack([first_cos[:half_rows], -first_sin[:half_rows]], axis=1)
    twist_even = jnp.concatenate([twist_cos, twist_cos], axis=1)
    twist_ahead = jnp.concatenate([twist_sin, -twist_sin], axis=1)
    twist_back = jnp.concatenate([-twist_sin, twist_sin], axis=1)
    block_ahead = jnp.concatenate(
        [
            jnp.concatenate([second_cos, -second_sin], axis=1),
            jnp.concatenate([second_sin, second_cos], axis=1),
        ],
        axis=0,
    )
    block_back = jnp.concatenate(
        [
            jnp.concatenate([second_cos, second_sin], axis=1),
            jnp.concatenate([-second_sin, second_cos], axis=1),
        ],
        axis=0,
    )
    kernel_spec = forward(
        kernel.reshape(group_size, factor, width_second),
        first_table,
        twist_even,
        twist_ahead,
        block_ahead,
    )
    data_spec = forward(
        spread.reshape(group_size, half_rows, width_second),
        first_table[:, :, :half_rows],
        twist_even,
        twist_ahead,
        block_ahead,
    )
    data_re = data_spec[..., :width_second]
    data_im = data_spec[..., width_second:]
    kernel_re = kernel_spec[..., :width_second]
    kernel_im = kernel_spec[..., width_second:]
    joined = jnp.concatenate(
        [data_re * kernel_re - data_im * kernel_im, data_re * kernel_im + data_im * kernel_re],
        axis=-1,
    )
    convolved = inverse(joined, last_table, twist_even, twist_back, block_back, span_len).reshape(
        group_size, seq_len
    )
    returned = lax.all_to_all(convolved, "col", split_axis=1, concat_axis=0, tiled=True)
    mixed_rows = ((returned.T + skip_gain * product) * gate_part).astype(jnp.bfloat16)
    return jnp.dot(mixed_rows, out_weight, preferred_element_type=jnp.float32).astype(jnp.bfloat16)[
        None
    ]


f32, bf16 = (jnp.float32, jnp.bfloat16)
EDGE = 16


def wave_tables(seq_len):
    odd = 2 * np.arange(seq_len, dtype=np.int64) + 1
    angle = (odd[:, None] * odd[None, :] % (8 * seq_len)) * (math.pi / (4 * seq_len))
    pieces = []
    for table in (np.cos(angle), np.sin(angle)):
        high = table.astype(bf16)
        pieces += [high, (table - high.astype(np.float64)).astype(bf16)]
    half = odd * (math.pi / (4 * seq_len))
    turn = np.stack([np.cos(half), np.sin(half)]).astype(np.float32)
    turn = np.repeat(turn[:, :, None], 128, axis=2)
    return (np.stack(pieces), turn)


def feature_table(seq_len, feature_count):
    position = np.arange(seq_len, dtype=np.float64)
    bands = (feature_count - 1) // 2
    values = np.linspace(0.0001, bands - 1, bands)
    angles = (2.0 * math.pi / seq_len * position)[:, None] * values[None, :]
    tau = position / (seq_len - 1)
    table = np.concatenate([tau[:, None], np.cos(angles), -np.sin(angles)], axis=1)
    return np.pad(table, ((0, 0), (0, 128 - feature_count))).astype(np.float32)


def sine(x):
    turns = jnp.floor(x * (1.0 / math.pi) + 0.5)
    r = x - turns * 3.140625
    r = r - turns * 9.67502593994140625e-4
    r = r - turns * 1.509957990978376432e-7
    sign = 1.0 - 2.0 * (turns - 2.0 * jnp.floor(turns * 0.5))
    s = r * r
    poly = 1.0 / 362880.0 - s * (1.0 / 39916800.0)
    poly = -1.0 / 5040.0 + s * poly
    poly = 1.0 / 120.0 + s * poly
    poly = -1.0 / 6.0 + s * poly
    return sign * (r + r * s * poly)


def split(value):
    high = value.astype(bf16)
    return (high, (value - high.astype(f32)).astype(bf16))


def mul(a, b):
    return jnp.dot(a, b, preferred_element_type=f32)


def mul_precise(a, b):
    return jnp.dot(a, b, preferred_element_type=f32, precision=highest)


def neighbours(rows, before, after):
    count = rows.shape[0]
    index = lax.broadcasted_iota(jnp.int32, rows.shape, 0)
    up = jnp.where(index == 0, before, pltpu.roll(rows, 1, 0))
    down = jnp.where(index == count - 1, after, pltpu.roll(rows, count - 1, 0))
    return (up, down)


def short_form(rows, taps, before, after):
    up, down = neighbours(rows, before, after)
    return taps[0:1] * up + taps[1:2] * rows + taps[2:3] * down


def conv_kernel(
    n,
    gate_hbm,
    mult_hbm,
    value_hbm,
    taps_gate_hbm,
    taps_mult_hbm,
    taps_value_hbm,
    first_hbm,
    second_hbm,
    ahead_hbm,
    behind_hbm,
    decay_hbm,
    skip_hbm,
    weight_hbm,
    table_hbm,
    turn_hbm,
    feature_hbm,
    out_ref,
    gate,
    mult,
    value,
    taps_gate,
    taps_mult,
    taps_value,
    second_ref,
    decay_ref,
    skip_ref,
    first,
    ahead_w,
    behind_w,
    weight,
    table,
    turn,
    feature,
    sent,
    came,
    whole,
    back_sent,
    back_came,
    halo_sent,
    halo_came,
    kernel_re,
    kernel_im,
    spec,
    gate_part,
    direct,
    total,
    load_sems,
    send_sems,
    recv_sems,
    back_send,
    back_recv,
    halo_send,
    halo_recv,
):
    me = lax.axis_index("col")
    rows, channels = gate.shape
    group = channels // n
    seq_len = rows * n
    near = me + 1 - 2 * lax.rem(me, 2)
    peers = []
    for j in range(1, n // 2):
        peers += [lax.rem(me + 2 * j, n), lax.rem(near + 2 * j, n)]
    peers.append(near)

    def columns(owner):
        return pl.ds(pl.multiple_of(owner * group, group), group)

    loads = [
        pltpu.make_async_copy(s, d, load_sems.at[i])
        for i, (s, d) in enumerate(
            [
                (value_hbm.at[0], value),
                (mult_hbm.at[0], mult),
                (taps_value_hbm, taps_value),
                (taps_mult_hbm, taps_mult),
                (feature_hbm, feature),
                (first_hbm, first.at[pl.ds(0, first_hbm.shape[0])]),
                (second_hbm, second_ref),
                (decay_hbm, decay_ref),
                (ahead_hbm.at[:, columns(me)], ahead_w),
                (behind_hbm.at[:, columns(me)], behind_w),
                (table_hbm, table),
                (turn_hbm, turn),
                (gate_hbm.at[0], gate),
                (taps_gate_hbm, taps_gate),
                (skip_hbm, skip_ref),
                (weight_hbm, weight),
            ]
        )
    ]
    for load in loads:
        load.start()
    barrier = pltpu.get_barrier_semaphore()
    for peer in peers:
        pl.semaphore_signal(
            barrier, inc=1, device_id={"col": peer}, device_id_type=pl.DeviceIdType.MESH
        )
    for load in loads[:4]:
        load.wait()

    def pack(owner):
        cols = columns(owner)
        v = value[:, cols].astype(f32)
        m = mult[:, cols].astype(f32)
        zero = jnp.zeros((1, group), f32)
        vs = short_form(v, taps_value[:, cols], zero, zero)
        ms = short_form(m, taps_mult[:, cols], zero, zero)
        sent[owner, pl.ds(0, rows), :] = (vs * ms).astype(bf16)
        edges = jnp.concatenate(
            [v[0:2], v[rows - 2 : rows], m[0:2], m[rows - 2 : rows], jnp.zeros((8, group), f32)], axis=0
        )
        sent[owner, pl.ds(rows, EDGE), :] = edges.astype(bf16)

    def remote(src, dst, ssem, rsem, peer):
        return pltpu.make_async_remote_copy(
            src_ref=src,
            dst_ref=dst,
            send_sem=ssem,
            recv_sem=rsem,
            device_id={"col": peer},
            device_id_type=pl.DeviceIdType.MESH,
        )

    copies = []
    for i, peer in enumerate(peers):
        pack(peer)
        if i == 0:
            pl.semaphore_wait(barrier, n - 1)
        copy = remote(sent.at[peer], came.at[me], send_sems.at[peer], recv_sems.at[me], peer)
        copy.start()
        copies.append(copy)
    loads[12].wait()
    right, left = (lax.rem(me + 1, n), lax.rem(me + n - 1, n))
    for side, (row, target) in enumerate([(rows - 1, right), (0, left)]):
        base = rows - EDGE if row else 0
        at = row - base
        parts = [r[base : base + EDGE, :].astype(f32)[at : at + 1] for r in (gate, mult, value)]
        tile = jnp.concatenate(parts + [jnp.zeros((EDGE - 3, channels), f32)], axis=0)
        halo_sent[side] = tile.astype(bf16)
        copy = remote(
            halo_sent.at[side], halo_came.at[side], halo_send.at[side], halo_recv.at[side], target
        )
        copy.start()
        copies.append(copy)
    pack(me)

    for load in loads[4:10]:
        load.wait()
    used = first_hbm.shape[0]
    at = lax.broadcasted_iota(jnp.int32, first.shape, 0)
    first_w = jnp.where(at < used, first[...], 0.0)
    hidden = sine(mul_precise(feature[...], first_w))
    hidden = sine(mul_precise(hidden, second_ref[...]))
    later = pltpu.roll(hidden, seq_len - 1, 0)
    rates = decay_ref[:, columns(me)]
    index = lax.broadcasted_iota(jnp.int32, (seq_len, group), 0)
    tau = index.astype(f32) * (1.0 / (seq_len - 1))
    fade = jnp.exp(-rates * tau)
    step = jnp.exp(-rates * (1.0 / (seq_len - 1)))
    ahead = mul_precise(hidden, ahead_w[...]) * fade
    behind = mul_precise(later, behind_w[...]) * (fade * step)
    behind = jnp.where(index == seq_len - 1, 0.0, behind)
    power = jnp.sum(ahead * ahead + behind * behind, axis=0, keepdims=True)
    scale = lax.rsqrt(power + 1e-06) * (2.0 / (2 * seq_len))
    loads[10].wait()
    loads[11].wait()
    high, low = split((ahead + behind) * scale)
    even = mul(table[0], high) + mul(table[1], high) + mul(table[0], low)
    high, low = split((ahead - behind) * scale)
    odd = mul(table[2], high) + mul(table[3], high) + mul(table[2], low)
    cos_half = turn[0][:, 0:1]
    sin_half = turn[1][:, 0:1]
    kernel_re[...] = cos_half * even + sin_half * odd
    kernel_im[...] = sin_half * even - cos_half * odd

    whole[pl.ds(pl.multiple_of(me * rows, rows), rows), :] = sent[me, pl.ds(0, rows), :]
    came[me, pl.ds(rows, EDGE), :] = sent[me, pl.ds(rows, EDGE), :]
    for peer in reversed(peers):
        remote(sent.at[peer], came.at[peer], send_sems.at[peer], recv_sems.at[peer], peer).wait_recv()
        whole[pl.ds(pl.multiple_of(peer * rows, rows), rows), :] = came[peer, pl.ds(0, rows), :]
    edges = [came[s, pl.ds(rows, EDGE), :].astype(f32) for s in range(n)]
    own_taps = [t[:, columns(me)] for t in (taps_value, taps_mult)]
    tile_at = lax.broadcasted_iota(jnp.int32, (EDGE, group), 0)
    for s in range(n):
        top = bottom = 1.0
        for k, taps in enumerate(own_taps):
            e = edges[s][4 * k : 4 * k + 4]
            first_row = taps[1:2] * e[0:1] + taps[2:3] * e[1:2]
            last_row = taps[0:1] * e[2:3] + taps[1:2] * e[3:4]
            if s > 0:
                first_row += taps[0:1] * edges[s - 1][4 * k + 3 : 4 * k + 4]
            if s < n - 1:
                last_row += taps[2:3] * edges[s + 1][4 * k : 4 * k + 1]
            top, bottom = (top * first_row, bottom * last_row)
        for base, at, row in ((s * rows, 0, top), ((s + 1) * rows - EDGE, EDGE - 1, bottom)):
            old = whole[base : base + EDGE, :].astype(f32)
            whole[base : base + EDGE, :] = jnp.where(tile_at == at, row, old).astype(bf16)

    x = whole[...]
    xc = mul(table[0], x) + mul(table[1], x)
    xs = mul(table[2], x) + mul(table[3], x)
    kr, ki = (kernel_re[...], kernel_im[...])
    spec[0], spec[1] = split(xc * kr + xs * ki)
    spec[2], spec[3] = split(xs * kr - xc * ki)

    def invert(owner):
        take = pl.ds(pl.multiple_of(owner * rows, rows), rows)
        ch, cl, sh, sl = (table[i, take, :] for i in range(4))
        return (
            mul(ch, spec[0]) + mul(sh, spec[2])
            + mul(cl, spec[0]) + mul(sl, spec[2])
            + mul(ch, spec[1]) + mul(sh, spec[3])
        )

    for peer in peers:
        back_sent[peer] = invert(peer).astype(bf16)
        copy = remote(
            back_sent.at[peer], back_came.at[me], back_send.at[peer], back_recv.at[me], peer
        )
        copy.start()
        copies.append(copy)
    own_back = invert(me)

    for side, target in enumerate((left, right)):
        remote(
            halo_sent.at[side], halo_came.at[side], halo_send.at[side], halo_recv.at[side], target
        ).wait_recv()
    loads[13].wait()
    loads[14].wait()
    has_left = (me > 0).astype(f32)
    has_right = (me < n - 1).astype(f32)
    for s in range(n):
        cols = slice(s * group, (s + 1) * group)
        before = halo_came[0, :, cols].astype(f32) * has_left
        after = halo_came[1, :, cols].astype(f32) * has_right
        parts = []
        for i, (r, taps) in enumerate(((gate, taps_gate), (mult, taps_mult), (value, taps_value))):
            parts.append(
                short_form(r[:, cols].astype(f32), taps[:, cols], before[i : i + 1], after[i : i + 1])
            )
        gate_part[s] = parts[0]
        direct[s] = skip_ref[:, cols] * (parts[1] * parts[2])
    loads[15].wait()

    def project(owner, convolved):
        gated = ((convolved + direct[owner]) * gate_part[owner]).astype(bf16)
        return mul(gated, weight[columns(owner), :])

    total[...] = project(me, own_back)
    for i, peer in enumerate(reversed(peers)):
        remote(
            back_sent.at[peer], back_came.at[peer], back_send.at[peer], back_recv.at[peer], peer
        ).wait_recv()
        term = project(peer, back_came[peer].astype(f32))
        if i < n - 2:
            total[...] += term
        else:
            out_ref[0] = (total[...] + term).astype(bf16)
    for copy in copies:
        copy.wait_send()


def fused_body(n, *args):
    gate_in, mult_in, value_in, tg, tm, tv, first, second, ahead, behind, decay, skip, weight = args
    _, rows, channels = gate_in.shape
    seq_len, group = (rows * n, channels // n)
    width = weight.shape[1]
    tables, turn = wave_tables(seq_len)
    features = feature_table(seq_len, first.shape[0])
    vmem = pl.BlockSpec(memory_space=pltpu.VMEM)
    main = pl.BlockSpec(memory_space=pltpu.HBM)
    hidden_count = second.shape[0]
    dma = pltpu.SemaphoreType.DMA
    return pl.pallas_call(
        functools.partial(conv_kernel, n),
        out_shape=jax.ShapeDtypeStruct((1, rows, width), bf16),
        in_specs=[main] * 16,
        out_specs=vmem,
        scratch_shapes=[
            pltpu.VMEM((rows, channels), bf16),
            pltpu.VMEM((rows, channels), bf16),
            pltpu.VMEM((rows, channels), bf16),
            pltpu.VMEM(tg.shape, f32),
            pltpu.VMEM(tm.shape, f32),
            pltpu.VMEM(tv.shape, f32),
            pltpu.VMEM(second.shape, f32),
            pltpu.VMEM((1, channels), f32),
            pltpu.VMEM((1, channels), f32),
            pltpu.VMEM((128, hidden_count), f32),
            pltpu.VMEM((hidden_count, group), f32),
            pltpu.VMEM((hidden_count, group), f32),
            pltpu.VMEM(weight.shape, bf16),
            pltpu.VMEM(tables.shape, bf16),
            pltpu.VMEM(turn.shape, f32),
            pltpu.VMEM(features.shape, f32),
            pltpu.VMEM((n, rows + EDGE, group), bf16),
            pltpu.VMEM((n, rows + EDGE, group), bf16),
            pltpu.VMEM((seq_len, group), bf16),
            pltpu.VMEM((n, rows, group), bf16),
            pltpu.VMEM((n, rows, group), bf16),
            pltpu.VMEM((2, EDGE, channels), bf16),
            pltpu.VMEM((2, EDGE, channels), bf16),
            pltpu.VMEM((seq_len, group), f32),
            pltpu.VMEM((seq_len, group), f32),
            pltpu.VMEM((4, seq_len, group), bf16),
            pltpu.VMEM((n, rows, group), f32),
            pltpu.VMEM((n, rows, group), f32),
            pltpu.VMEM((rows, width), f32),
            dma((16,)),
            dma((n,)),
            dma((n,)),
            dma((n,)),
            dma((n,)),
            dma((2,)),
            dma((2,)),
        ],
        compiler_params=pltpu.CompilerParams(
            collective_id=0, has_side_effects=True
        ),
    )(
        gate_in, mult_in, value_in, tg, tm, tv, first, second, ahead, behind,
        decay.reshape(1, channels), skip.reshape(1, channels), weight,
        jnp.asarray(tables), jnp.asarray(turn), jnp.asarray(features),
    )


def body_for(n, *args):
    _, rows, channels = args[0].shape
    small = rows * n <= 1024 and rows % 128 == 0 and channels % (128 * n) == 0
    network = args[6].shape[0] <= 128 and args[6].shape[1] == 128
    if n >= 2 and n % 2 == 0 and small and network and args[3].shape[0] == 3:
        return fused_body(n, *args)
    return spread_body(*args)


def solution(mesh):
    in_specs = (
        P(("grp", "row"), "col", None),
        P(("grp", "row"), "col", None),
        P(("grp", "row"), "col", None),
        P(),
        P(),
        P(),
        P(),
        P(),
        P(),
        P(),
        P(),
        P(),
        P(),
    )
    out_specs = P(("grp", "row"), "col", None)

    body = functools.partial(body_for, mesh.shape["col"])
    return jax.shard_map(body, mesh=mesh, in_specs=in_specs, out_specs=out_specs, check_vma=False)
```

```python
import functools
import math

import jax
import jax.numpy as jnp
import numpy as np
from jax import lax
from jax.experimental import pallas as pl
from jax.experimental.pallas import tpu as pltpu
from jax.sharding import PartitionSpec as P

highest = lax.Precision.HIGHEST


def padded_2(shard, sides, width):
    for axis, dim in sides:
        size, length = (lax.axis_size(axis), shard.shape[dim])
        up = [(i, (i + 1) % size) for i in range(size - 1)]
        down = [(j, i) for i, j in up]
        last = lax.slice_in_dim(shard, length - width, length, axis=dim)
        leading = lax.slice_in_dim(shard, 0, width, axis=dim)
        before = lax.ppermute(last, axis, up)
        after = lax.ppermute(leading, axis, down)
        shard = jnp.concatenate([before, shard, after], axis=dim)
    return shard


def filter_hidden(mirror, seq_len, filter_first, filter_second):
    tau_values = mirror.astype(jnp.float32) / (seq_len - 1)
    omega_pos = 2.0 * math.pi / seq_len * mirror.astype(jnp.float32)
    band_count = (filter_first.shape[0] - 1) // 2
    band_values = jnp.linspace(0.0001, band_count - 1, band_count, dtype=jnp.float32)
    angles = omega_pos[:, None] * band_values[None, :]
    features = jnp.concatenate([tau_values[:, None], jnp.cos(angles), -jnp.sin(angles)], axis=1)
    hidden = jnp.sin(jnp.dot(features, filter_first, precision=highest))
    hidden = jnp.sin(jnp.dot(hidden, filter_second, precision=highest))
    return (hidden, tau_values)


def side_values(hidden, tau_values, side_weight, decay_rates):
    values = jnp.einsum("pf,fh->hp", hidden, side_weight, precision=highest)
    return values * jnp.exp(-decay_rates[:, None] * tau_values[None, :])


def angle_table(row_count, column_count, period):
    products = (
        lax.iota(jnp.int32, row_count)[:, None]
        * lax.iota(jnp.int32, column_count)[None, :]
        % period
    )
    angle = products.astype(jnp.float32) * (2.0 * math.pi / period)
    return (jnp.cos(angle), jnp.sin(angle))


def swap_halves(stacked, width):
    return jnp.concatenate([stacked[..., width:], stacked[..., :width]], axis=-1)


def forward(values, first_table, twist_even, twist_odd, second_block):
    channels, _, width = values.shape
    first = jnp.einsum("sfa,cab->cfsb", first_table, values, precision=highest)
    first = first.reshape(channels, first_table.shape[1], 2 * width)
    turned = first * twist_even + swap_halves(first, width) * twist_odd
    return jnp.einsum("cfk,kl->cfl", turned, second_block, precision=highest)


def inverse(spectrum, last_table, twist_even, twist_odd, second_block, span_len):
    channels, freq_rows, double_width = spectrum.shape
    width = double_width // 2
    back = jnp.einsum("cfk,kl->cfl", spectrum, second_block, precision=highest)
    turned = back * twist_even + swap_halves(back, width) * twist_odd
    turned = turned.reshape(channels, freq_rows, 2, width)
    result = jnp.einsum("asf,cfsb->cab", last_table, turned, precision=highest)
    return result / span_len


def spread_body(
    gate_in,
    mult_in,
    value_in,
    taps_gate,
    taps_mult,
    taps_value,
    filter_first,
    filter_second,
    filter_ahead,
    filter_behind,
    filter_decay,
    skip_gain,
    out_weight,
):
    col_count = lax.axis_size("col")
    col_index = lax.axis_index("col")
    tok_rows = gate_in.shape[1]
    seq_len = tok_rows * col_count
    span_len = 2 * seq_len
    group_size = filter_ahead.shape[1] // col_count
    stacked = jnp.stack([gate_in[0], mult_in[0], value_in[0]])
    padded = padded_2(stacked, (("col", 1),), 1).astype(jnp.float32)
    all_taps = jnp.stack([taps_gate, taps_mult, taps_value])
    shorted = jnp.zeros(stacked.shape, jnp.float32)
    for offset in range(all_taps.shape[1]):
        shorted = shorted + all_taps[:, offset][:, None, :] * padded[:, offset : offset + tok_rows]
    gate_part = shorted[0]
    product = shorted[2] * shorted[1]
    spread = lax.all_to_all(product.T, "col", split_axis=0, concat_axis=1, tiled=True)
    first_channel = col_index * group_size
    own_rates = lax.dynamic_slice_in_dim(filter_decay, first_channel, group_size)
    mirror = lax.iota(jnp.int32, seq_len)
    hidden, tau_values = filter_hidden(mirror, seq_len, filter_first, filter_second)
    ahead_vals = side_values(
        hidden,
        tau_values,
        lax.dynamic_slice_in_dim(filter_ahead, first_channel, group_size, 1),
        own_rates,
    )
    behind_vals = side_values(
        hidden,
        tau_values,
        lax.dynamic_slice_in_dim(filter_behind, first_channel, group_size, 1),
        own_rates,
    )
    kernel = jnp.concatenate(
        [ahead_vals, jnp.zeros((group_size, 1), jnp.float32), jnp.flip(behind_vals[:, 1:], axis=1)],
        axis=1,
    )
    kernel = kernel * lax.rsqrt(jnp.sum(kernel * kernel, axis=1, keepdims=True) + 1e-06)
    factor = 128
    half_rows = factor // 2
    width_second = span_len // factor
    first_cos, first_sin = angle_table(factor, factor, factor)
    twist_cos, twist_sin = angle_table(factor, width_second, span_len)
    second_cos, second_sin = angle_table(width_second, width_second, width_second)
    first_table = jnp.stack([first_cos, -first_sin])
    last_table = jnp.stack([first_cos[:half_rows], -first_sin[:half_rows]], axis=1)
    twist_even = jnp.concatenate([twist_cos, twist_cos], axis=1)
    twist_ahead = jnp.concatenate([twist_sin, -twist_sin], axis=1)
    twist_back = jnp.concatenate([-twist_sin, twist_sin], axis=1)
    block_ahead = jnp.concatenate(
        [
            jnp.concatenate([second_cos, -second_sin], axis=1),
            jnp.concatenate([second_sin, second_cos], axis=1),
        ],
        axis=0,
    )
    block_back = jnp.concatenate(
        [
            jnp.concatenate([second_cos, second_sin], axis=1),
            jnp.concatenate([-second_sin, second_cos], axis=1),
        ],
        axis=0,
    )
    kernel_spec = forward(
        kernel.reshape(group_size, factor, width_second),
        first_table,
        twist_even,
        twist_ahead,
        block_ahead,
    )
    data_spec = forward(
        spread.reshape(group_size, half_rows, width_second),
        first_table[:, :, :half_rows],
        twist_even,
        twist_ahead,
        block_ahead,
    )
    data_re = data_spec[..., :width_second]
    data_im = data_spec[..., width_second:]
    kernel_re = kernel_spec[..., :width_second]
    kernel_im = kernel_spec[..., width_second:]
    joined = jnp.concatenate(
        [data_re * kernel_re - data_im * kernel_im, data_re * kernel_im + data_im * kernel_re],
        axis=-1,
    )
    convolved = inverse(joined, last_table, twist_even, twist_back, block_back, span_len).reshape(
        group_size, seq_len
    )
    returned = lax.all_to_all(convolved, "col", split_axis=1, concat_axis=0, tiled=True)
    mixed_rows = ((returned.T + skip_gain * product) * gate_part).astype(jnp.bfloat16)
    return jnp.dot(mixed_rows, out_weight, preferred_element_type=jnp.float32).astype(jnp.bfloat16)[
        None
    ]


f32, bf16 = (jnp.float32, jnp.bfloat16)
EDGE = 16
PARTS = 2


def wave_tables(seq_len):
    odd = 2 * np.arange(seq_len, dtype=np.int64) + 1
    angle = (odd[:, None] * odd[None, :] % (8 * seq_len)) * (math.pi / (4 * seq_len))
    pieces = []
    for table in (np.cos(angle), np.sin(angle)):
        high = table.astype(bf16)
        pieces += [high, (table - high.astype(np.float64)).astype(bf16)]
    half = odd * (math.pi / (4 * seq_len))
    turn = np.stack([np.cos(half), np.sin(half)]).astype(np.float32)
    turn = np.repeat(turn[:, :, None], 128, axis=2)
    return (np.stack(pieces), turn)


def feature_table(seq_len, feature_count):
    position = np.arange(seq_len, dtype=np.float64)
    bands = (feature_count - 1) // 2
    values = np.linspace(0.0001, bands - 1, bands)
    angles = (2.0 * math.pi / seq_len * position)[:, None] * values[None, :]
    tau = position / (seq_len - 1)
    table = np.concatenate([tau[:, None], np.cos(angles), -np.sin(angles)], axis=1)
    return np.pad(table, ((0, 0), (0, 128 - feature_count))).astype(np.float32)


def sine(x):
    turns = jnp.floor(x * (1.0 / math.pi) + 0.5)
    r = x - turns * 3.140625
    r = r - turns * 9.67502593994140625e-4
    r = r - turns * 1.509957990978376432e-7
    sign = 1.0 - 2.0 * (turns - 2.0 * jnp.floor(turns * 0.5))
    s = r * r
    poly = 1.0 / 362880.0 - s * (1.0 / 39916800.0)
    poly = -1.0 / 5040.0 + s * poly
    poly = 1.0 / 120.0 + s * poly
    poly = -1.0 / 6.0 + s * poly
    return sign * (r + r * s * poly)


def split(value):
    high = value.astype(bf16)
    return (high, (value - high.astype(f32)).astype(bf16))


def mul(a, b):
    return jnp.dot(a, b, preferred_element_type=f32)


def mul_precise(a, b):
    return jnp.dot(a, b, preferred_element_type=f32, precision=highest)


def neighbours(rows, before, after):
    count = rows.shape[0]
    index = lax.broadcasted_iota(jnp.int32, rows.shape, 0)
    up = jnp.where(index == 0, before, pltpu.roll(rows, 1, 0))
    down = jnp.where(index == count - 1, after, pltpu.roll(rows, count - 1, 0))
    return (up, down)


def short_form(rows, taps, before, after):
    up, down = neighbours(rows, before, after)
    return taps[0:1] * up + taps[1:2] * rows + taps[2:3] * down


def conv_kernel(
    n,
    gate_hbm,
    mult_hbm,
    value_hbm,
    taps_gate_hbm,
    taps_mult_hbm,
    taps_value_hbm,
    first_hbm,
    second_hbm,
    ahead_hbm,
    behind_hbm,
    decay_hbm,
    skip_hbm,
    weight_hbm,
    table_hbm,
    turn_hbm,
    feature_hbm,
    out_ref,
    gate,
    mult,
    value,
    taps_gate,
    taps_mult,
    taps_value,
    second_ref,
    decay_ref,
    skip_ref,
    first,
    ahead_w,
    behind_w,
    weight,
    table,
    turn,
    feature,
    sent,
    came,
    whole,
    back_sent,
    back_came,
    halo_sent,
    halo_came,
    kernel_re,
    kernel_im,
    spec,
    gate_part,
    direct,
    total,
    load_sems,
    send_sems,
    recv_sems,
    back_send,
    back_recv,
    halo_send,
    halo_recv,
):
    me = lax.axis_index("col")
    rows, channels = gate.shape
    group = channels // n
    seq_len = rows * n
    near = me + 1 - 2 * lax.rem(me, 2)
    peers = []
    for j in range(1, n // 2):
        peers += [lax.rem(me + 2 * j, n), lax.rem(near + 2 * j, n)]
    peers.append(near)

    def columns(owner):
        return pl.ds(pl.multiple_of(owner * group, group), group)

    loads = [
        pltpu.make_async_copy(s, d, load_sems.at[i])
        for i, (s, d) in enumerate(
            [
                (value_hbm.at[0], value),
                (mult_hbm.at[0], mult),
                (taps_value_hbm, taps_value),
                (taps_mult_hbm, taps_mult),
                (feature_hbm, feature),
                (first_hbm, first.at[pl.ds(0, first_hbm.shape[0])]),
                (second_hbm, second_ref),
                (decay_hbm, decay_ref),
                (ahead_hbm.at[:, columns(me)], ahead_w),
                (behind_hbm.at[:, columns(me)], behind_w),
                (table_hbm, table),
                (turn_hbm, turn),
                (gate_hbm.at[0], gate),
                (taps_gate_hbm, taps_gate),
                (skip_hbm, skip_ref),
                (weight_hbm, weight),
            ]
        )
    ]
    for load in loads:
        load.start()
    barrier = pltpu.get_barrier_semaphore()
    for peer in peers:
        pl.semaphore_signal(
            barrier, inc=1, device_id={"col": peer}, device_id_type=pl.DeviceIdType.MESH
        )
    for load in loads[:4]:
        load.wait()

    part = group // PARTS

    def piece(owner, h):
        return pl.ds(pl.multiple_of(owner * group + h * part, part), part)

    def pack(owner, h):
        cols = piece(owner, h)
        v = value[:, cols].astype(f32)
        m = mult[:, cols].astype(f32)
        zero = jnp.zeros((1, part), f32)
        vs = short_form(v, taps_value[:, cols], zero, zero)
        ms = short_form(m, taps_mult[:, cols], zero, zero)
        sent[h, owner, pl.ds(0, rows), :] = (vs * ms).astype(bf16)
        edges = jnp.concatenate(
            [v[0:2], v[rows - 2 : rows], m[0:2], m[rows - 2 : rows], jnp.zeros((8, part), f32)], axis=0
        )
        sent[h, owner, pl.ds(rows, EDGE), :] = edges.astype(bf16)

    def remote(src, dst, ssem, rsem, peer):
        return pltpu.make_async_remote_copy(
            src_ref=src,
            dst_ref=dst,
            send_sem=ssem,
            recv_sem=rsem,
            device_id={"col": peer},
            device_id_type=pl.DeviceIdType.MESH,
        )

    copies = []
    for h in range(PARTS):
        for i, peer in enumerate(peers):
            pack(peer, h)
            if i + h == 0:
                pl.semaphore_wait(barrier, n - 1)
            copy = remote(
                sent.at[h, peer], came.at[h, me], send_sems.at[h, peer], recv_sems.at[h, me], peer
            )
            copy.start()
            copies.append(copy)
    loads[12].wait()
    right, left = (lax.rem(me + 1, n), lax.rem(me + n - 1, n))
    for side, (row, target) in enumerate([(rows - 1, right), (0, left)]):
        base = rows - EDGE if row else 0
        at = row - base
        parts = [r[base : base + EDGE, :].astype(f32)[at : at + 1] for r in (gate, mult, value)]
        tile = jnp.concatenate(parts + [jnp.zeros((EDGE - 3, channels), f32)], axis=0)
        halo_sent[side] = tile.astype(bf16)
        copy = remote(
            halo_sent.at[side], halo_came.at[side], halo_send.at[side], halo_recv.at[side], target
        )
        copy.start()
        copies.append(copy)
    for h in range(PARTS):
        pack(me, h)

    for load in loads[4:10]:
        load.wait()
    used = first_hbm.shape[0]
    at = lax.broadcasted_iota(jnp.int32, first.shape, 0)
    first_w = jnp.where(at < used, first[...], 0.0)
    hidden = sine(mul_precise(feature[...], first_w))
    hidden = sine(mul_precise(hidden, second_ref[...]))
    later = pltpu.roll(hidden, seq_len - 1, 0)
    rates = decay_ref[:, columns(me)]
    index = lax.broadcasted_iota(jnp.int32, (seq_len, group), 0)
    tau = index.astype(f32) * (1.0 / (seq_len - 1))
    fade = jnp.exp(-rates * tau)
    step = jnp.exp(-rates * (1.0 / (seq_len - 1)))
    ahead = mul_precise(hidden, ahead_w[...]) * fade
    behind = mul_precise(later, behind_w[...]) * (fade * step)
    behind = jnp.where(index == seq_len - 1, 0.0, behind)
    power = jnp.sum(ahead * ahead + behind * behind, axis=0, keepdims=True)
    scale = lax.rsqrt(power + 1e-06) * (2.0 / (2 * seq_len))
    loads[10].wait()
    loads[11].wait()
    high, low = split((ahead + behind) * scale)
    even = mul(table[0], high) + mul(table[1], high) + mul(table[0], low)
    high, low = split((ahead - behind) * scale)
    odd = mul(table[2], high) + mul(table[3], high) + mul(table[2], low)
    cos_half = turn[0][:, 0:1]
    sin_half = turn[1][:, 0:1]
    kernel_re[...] = cos_half * even + sin_half * odd
    kernel_im[...] = sin_half * even - cos_half * odd


    def near_product(h):
        whole[h, pl.ds(pl.multiple_of(me * rows, rows), rows), :] = sent[h, me, pl.ds(0, rows), :]
        came[h, me, pl.ds(rows, EDGE), :] = sent[h, me, pl.ds(rows, EDGE), :]
        for peer in reversed(peers):
            remote(
                sent.at[h, peer], came.at[h, peer], send_sems.at[h, peer], recv_sems.at[h, peer], peer
            ).wait_recv()
            whole[h, pl.ds(pl.multiple_of(peer * rows, rows), rows), :] = came[
                h, peer, pl.ds(0, rows), :
            ]
        edges = [came[h, s, pl.ds(rows, EDGE), :].astype(f32) for s in range(n)]
        own_taps = [t[:, piece(me, h)] for t in (taps_value, taps_mult)]
        tile_at = lax.broadcasted_iota(jnp.int32, (EDGE, part), 0)
        for s in range(n):
            top = bottom = 1.0
            for k, taps in enumerate(own_taps):
                e = edges[s][4 * k : 4 * k + 4]
                first_row = taps[1:2] * e[0:1] + taps[2:3] * e[1:2]
                last_row = taps[0:1] * e[2:3] + taps[1:2] * e[3:4]
                if s > 0:
                    first_row += taps[0:1] * edges[s - 1][4 * k + 3 : 4 * k + 4]
                if s < n - 1:
                    last_row += taps[2:3] * edges[s + 1][4 * k : 4 * k + 1]
                top, bottom = (top * first_row, bottom * last_row)
            for base, at, row in ((s * rows, 0, top), ((s + 1) * rows - EDGE, EDGE - 1, bottom)):
                old = whole[h, base : base + EDGE, :].astype(f32)
                whole[h, base : base + EDGE, :] = jnp.where(tile_at == at, row, old).astype(bf16)

    def invert(owner, h):
        take = pl.ds(pl.multiple_of(owner * rows, rows), rows)
        ch, cl, sh, sl = (table[i, take, :] for i in range(4))
        return (
            mul(ch, spec[h, 0]) + mul(sh, spec[h, 2])
            + mul(cl, spec[h, 0]) + mul(sl, spec[h, 2])
            + mul(ch, spec[h, 1]) + mul(sh, spec[h, 3])
        )

    for h in range(PARTS):
        near_product(h)
        x = whole[h]
        xc = mul(table[0], x) + mul(table[1], x)
        xs = mul(table[2], x) + mul(table[3], x)
        cols = slice(h * part, (h + 1) * part)
        kr, ki = (kernel_re[:, cols], kernel_im[:, cols])
        spec[h, 0], spec[h, 1] = split(xc * kr + xs * ki)
        spec[h, 2], spec[h, 3] = split(xs * kr - xc * ki)
        for peer in peers:
            back_sent[h, peer] = invert(peer, h).astype(bf16)
            copy = remote(
                back_sent.at[h, peer],
                back_came.at[h, me],
                back_send.at[h, peer],
                back_recv.at[h, me],
                peer,
            )
            copy.start()
            copies.append(copy)
    own_back = jnp.concatenate([invert(me, h) for h in range(PARTS)], axis=1)

    for side, target in enumerate((left, right)):
        remote(
            halo_sent.at[side], halo_came.at[side], halo_send.at[side], halo_recv.at[side], target
        ).wait_recv()
    loads[13].wait()
    loads[14].wait()
    has_left = (me > 0).astype(f32)
    has_right = (me < n - 1).astype(f32)
    for s in range(n):
        cols = slice(s * group, (s + 1) * group)
        before = halo_came[0, :, cols].astype(f32) * has_left
        after = halo_came[1, :, cols].astype(f32) * has_right
        parts = []
        for i, (r, taps) in enumerate(((gate, taps_gate), (mult, taps_mult), (value, taps_value))):
            parts.append(
                short_form(r[:, cols].astype(f32), taps[:, cols], before[i : i + 1], after[i : i + 1])
            )
        gate_part[s] = parts[0]
        direct[s] = skip_ref[:, cols] * (parts[1] * parts[2])
    loads[15].wait()

    def project(owner, convolved):
        gated = ((convolved + direct[owner]) * gate_part[owner]).astype(bf16)
        return mul(gated, weight[columns(owner), :])

    total[...] = project(me, own_back)
    for i, peer in enumerate(reversed(peers)):
        for h in range(PARTS):
            remote(
                back_sent.at[h, peer],
                back_came.at[h, peer],
                back_send.at[h, peer],
                back_recv.at[h, peer],
                peer,
            ).wait_recv()
        arrived = [back_came[h, peer].astype(f32) for h in range(PARTS)]
        term = project(peer, jnp.concatenate(arrived, axis=1))
        if i < n - 2:
            total[...] += term
        else:
            out_ref[0] = (total[...] + term).astype(bf16)
    for copy in copies:
        copy.wait_send()


def fused_body(n, *args):
    gate_in, mult_in, value_in, tg, tm, tv, first, second, ahead, behind, decay, skip, weight = args
    _, rows, channels = gate_in.shape
    seq_len, group = (rows * n, channels // n)
    width = weight.shape[1]
    part = group // PARTS
    tables, turn = wave_tables(seq_len)
    features = feature_table(seq_len, first.shape[0])
    vmem = pl.BlockSpec(memory_space=pltpu.VMEM)
    main = pl.BlockSpec(memory_space=pltpu.HBM)
    hidden_count = second.shape[0]
    dma = pltpu.SemaphoreType.DMA
    return pl.pallas_call(
        functools.partial(conv_kernel, n),
        out_shape=pltpu.VMEM((1, rows, width), bf16),
        in_specs=[main] * 16,
        out_specs=vmem,
        scratch_shapes=[
            pltpu.VMEM((rows, channels), bf16),
            pltpu.VMEM((rows, channels), bf16),
            pltpu.VMEM((rows, channels), bf16),
            pltpu.VMEM(tg.shape, f32),
            pltpu.VMEM(tm.shape, f32),
            pltpu.VMEM(tv.shape, f32),
            pltpu.VMEM(second.shape, f32),
            pltpu.VMEM((1, channels), f32),
            pltpu.VMEM((1, channels), f32),
            pltpu.VMEM((128, hidden_count), f32),
            pltpu.VMEM((hidden_count, group), f32),
            pltpu.VMEM((hidden_count, group), f32),
            pltpu.VMEM(weight.shape, bf16),
            pltpu.VMEM(tables.shape, bf16),
            pltpu.VMEM(turn.shape, f32),
            pltpu.VMEM(features.shape, f32),
            pltpu.VMEM((PARTS, n, rows + EDGE, part), bf16),
            pltpu.VMEM((PARTS, n, rows + EDGE, part), bf16),
            pltpu.VMEM((PARTS, seq_len, part), bf16),
            pltpu.VMEM((PARTS, n, rows, part), bf16),
            pltpu.VMEM((PARTS, n, rows, part), bf16),
            pltpu.VMEM((2, EDGE, channels), bf16),
            pltpu.VMEM((2, EDGE, channels), bf16),
            pltpu.VMEM((seq_len, group), f32),
            pltpu.VMEM((seq_len, group), f32),
            pltpu.VMEM((PARTS, 4, seq_len, part), bf16),
            pltpu.VMEM((n, rows, group), f32),
            pltpu.VMEM((n, rows, group), f32),
            pltpu.VMEM((rows, width), f32),
            dma((16,)),
            dma((PARTS, n)),
            dma((PARTS, n)),
            dma((PARTS, n)),
            dma((PARTS, n)),
            dma((2,)),
            dma((2,)),
        ],
        compiler_params=pltpu.CompilerParams(
            collective_id=0, has_side_effects=True, vmem_limit_bytes=61 * 1024 * 1024
        ),
    )(
        gate_in, mult_in, value_in, tg, tm, tv, first, second, ahead, behind,
        decay.reshape(1, channels), skip.reshape(1, channels), weight,
        jnp.asarray(tables), jnp.asarray(turn), jnp.asarray(features),
    )


def body_for(n, *args):
    _, rows, channels = args[0].shape
    small = rows * n <= 1024 and rows % 128 == 0 and channels % (128 * PARTS * n) == 0
    network = args[6].shape[0] <= 128 and args[6].shape[1] == 128
    if n >= 2 and n % 2 == 0 and small and network and args[3].shape[0] == 3:
        return fused_body(n, *args)
    return spread_body(*args)


def solution(mesh):
    in_specs = (
        P(("grp", "row"), "col", None),
        P(("grp", "row"), "col", None),
        P(("grp", "row"), "col", None),
        P(),
        P(),
        P(),
        P(),
        P(),
        P(),
        P(),
        P(),
        P(),
        P(),
    )
    out_specs = P(("grp", "row"), "col", None)

    body = functools.partial(body_for, mesh.shape["col"])
    return jax.shard_map(body, mesh=mesh, in_specs=in_specs, out_specs=out_specs, check_vma=False)
```
